32 devices in a mesh: ep: 8 (over z, y), tp: 4 (over x, core).
Axes of the slice: x: 2, y: 2, z: 4, core: 2. Of those that a mesh axis runs over, the one named last changes fastest.
Arguments:
- mixer_value: bfloat16 [4096, 2048], P('ep', 'tp'), may hold values from -1 to 2
- mixer_gate: bfloat16 [4096, 2048], P('ep', 'tp'), may hold values from -6 to 6
- mixer_taps: bfloat16 [31, 2048], P(None, 'tp'), may hold values from -60 to 60
- mixer_gain: bfloat16 [2048], P('tp'), may hold values from 0.099609375 to 1.8984375
- mixer_weight: bfloat16 [2048, 4096], P('tp'), may hold values from -0.125 to 0.125
- routed_input: bfloat16 [4096, 4096], P('ep'), may hold values from -6 to 6
- routed_gain: bfloat16 [4096], replicated, may hold values from 0.099609375 to 1.8984375
- expert_ids: int32 [4096, 2], P('ep'), may hold values from 0 to 7, all different within a row; in each aligned block of 128 rows (0 to 127, 128 to 255, ...) at most 40 rows name the same one
- route_share: float32 [4096, 2], P('ep'), may hold values from 0.2 to 1
- gate_weight: bfloat16 [8, 4096, 2048], P('ep', None, 'tp'), may hold values from -0.09375 to 0.09375
- up_weight: bfloat16 [8, 4096, 2048], P('ep', None, 'tp'), may hold values from -0.09375 to 0.09375
- down_weight: bfloat16 [8, 2048, 4096], P('ep', 'tp'), may hold values from -0.125 to 0.125
Outputs:
- mixer_result: bfloat16 [4096, 4096], P(('ep', 'tp'))
- routed_result: bfloat16 [4096, 4096], P(('ep', 'tp'))
The draws below stay inside these ranges and needn't reach their ends.
Inputs may be any that keep to these rules, and one draw needn't show every extreme that they name: `expert_ids`: the two numbers of a row differ. In each aligned block of 128 rows no expert is named by more than 40 rows, and in every draw some expert is named by exactly 40 rows of some block.
All inputs are finite; a program needn't handle non-finite values.
Results may differ from the reference program's by a relative error of at most 0.011.
Values may be sent and summed in bfloat16 or wider, within the bound.
A program may use at most 192 MiB of HBM per device.

```python
import math
import jax
import jax.numpy as jnp
import numpy as np
from jax import lax

WIDTH = 4096
CHANNELS = 2048
TAPS = 31
EXPERT_UNITS = 2048
CHOSEN = 2
ROUTE_DEV = 128
EXPERTS = 8
CAPACITY = 40
MIX_TOKENS = 4096
ROUTE_TOKENS = 4096
N_EP = 8
N_TP = 4


def draw_mixer_taps(key, part):
    first_key, second_key = jax.random.split(key)
    position = jnp.arange(CHANNELS).astype(jnp.float32) / CHANNELS
    rough = jax.random.uniform(second_key, (CHANNELS,), jnp.float32, 0.5, 2.0)
    factor = jnp.exp(jnp.log(10.0) * position) * rough
    base = jnp.clip(jax.random.normal(first_key, (TAPS, CHANNELS), jnp.float32), -5.0, 5.0) + 0.3
    return (base * factor / math.sqrt(TAPS)).astype(jnp.bfloat16)


def block_levels(own_key, shape, cuts, low, largest):
    level, own = 1.0, jax.random.fold_in(own_key, 6)
    for dim, blocks in cuts:
        draws = jnp.exp(jax.random.uniform(jax.random.fold_in(own, dim), (blocks,), jnp.float32, low / len(cuts), largest / len(cuts)))
        level = level * jnp.repeat(draws, shape[dim] // blocks).reshape([-1 if axis == dim else 1 for axis in range(len(shape))])
    return level


def assign_block(own_key, own, number, rows, number_of, top, bound, skew):
    ranking = jax.random.permutation(own_key, number_of)
    crowded, common = load_shares(number_of, rows * top, bound, skew, True), load_shares(number_of, rows * top, bound, skew, False)
    places = jnp.arange(number_of)

    def named(sizes, turn):
        used = int((sizes > 0).sum())
        fixed = max(1, used // 4)
        moved = fixed + (places - fixed + turn * (used - fixed)) % max(1, number_of - fixed)
        return jnp.zeros((number_of,), jnp.int32).at[ranking[jnp.where(places < fixed, places, moved)]].set(jnp.asarray(sizes, jnp.int32))

    sizes = jnp.where(number % 4 == 0, named(crowded, number // 4), named(common, number - number // 4 - 1))
    mixed = jax.random.permutation(jax.random.fold_in(own, 3), number_of)
    donor, taker = mixed[0:number_of // 2 * 2:2], mixed[1:number_of // 2 * 2:2]
    slack = jnp.minimum(sizes[donor] - 1, bound - sizes[taker]) // 2
    slack = jnp.where((donor == ranking[0]) | (taker == ranking[0]) | (sizes[taker] == 0), 0, jnp.maximum(slack, 0))
    moved = jax.random.randint(jax.random.fold_in(own, 4), (number_of // 2,), 0, 1 << 20) % (slack + 1)
    sizes = sizes.at[donor].add(-moved).at[taker].add(moved)
    labels = jnp.searchsorted(jnp.cumsum(sizes), jnp.arange(rows * top), side="right").astype(jnp.int32)
    grid = labels.reshape(top, rows).T
    grid = grid[jax.random.permutation(jax.random.fold_in(own, 1), rows)]
    turn = jax.random.randint(jax.random.fold_in(own, 2), (rows, 1), 0, top)
    return jnp.take_along_axis(grid, (jnp.arange(top)[None, :] + turn) % top, axis=1)


def load_shares(amount, total, most, slope, full):
    loads = [(1 << 20) // math.isqrt(standing ** slope) + 1 for standing in range(1, amount + 1)]
    largest = most if full else min(most, max(-(-total // amount), total * loads[0] // sum(loads)))
    least = 1 if total - largest >= amount - 1 else 0
    counts, spare = [largest] + [least] * (amount - 1), total - largest - least * (amount - 1)
    while spare > 0:
        free = [i for i in range(1, amount) if counts[i] < largest] or [i for i in range(1, amount) if counts[i] < most]
        pool, left = sum([loads[i] for i in free]), spare
        for i in free:
            more = min(most - counts[i], max(1, left * loads[i] // pool), spare)
            counts[i] = counts[i] + more
            spare = spare - more
    return np.array(counts)


def gaussian(rng, dims, deviation, most, cuts=(), kind=jnp.bfloat16):
    entries = deviation * jax.random.normal(rng, dims, jnp.float32)
    if cuts:
        entries = entries * block_levels(rng, dims, cuts, -0.22, 0.18)
    return jnp.clip(entries, -most, most).astype(kind)


def setup_inputs(seed: int = 0) -> dict:
    key_list = jax.random.split(jax.random.key(seed), 13)
    mixer_value = jnp.clip(-1.0 + 3.0 * jax.random.uniform(key_list[0], (MIX_TOKENS, CHANNELS), jnp.float32) ** block_levels(key_list[0], (MIX_TOKENS, CHANNELS), ((0, 8), (1, 4)), -0.2, 0.2), -1.0, 2.0).astype(jnp.bfloat16)
    mixer_gate = gaussian(key_list[1], (MIX_TOKENS, CHANNELS), 1.0, 6.0, ((0, 8), (1, 4)))
    mixer_taps = draw_mixer_taps(jax.random.fold_in(key_list[12], 71), 0)
    mixer_gain = jnp.clip(1.0 + 0.18 * jax.random.normal(key_list[3], (CHANNELS,), jnp.float32), 0.099609375, 1.8984375).astype(jnp.bfloat16)
    mixer_weight = gaussian(key_list[4], (CHANNELS, WIDTH), CHANNELS ** -0.5, 0.125, ((0, 4),))
    routed_input = gaussian(key_list[5], (ROUTE_TOKENS, WIDTH), 1.0, 6.0, ((0, 8),))
    routed_gain = jnp.clip(1.0 + 0.18 * jax.random.normal(key_list[6], (WIDTH,), jnp.float32), 0.099609375, 1.8984375).astype(jnp.bfloat16)
    expert_ids_keys = jax.random.split(jax.random.fold_in(key_list[7], 1), ROUTE_TOKENS // ROUTE_DEV)
    expert_ids_turns = jax.random.permutation(jax.random.fold_in(key_list[7], 3), ROUTE_TOKENS // ROUTE_DEV)
    expert_ids = jax.vmap(lambda own, number: assign_block(jax.random.fold_in(key_list[7], 2), own, number, ROUTE_DEV, EXPERTS, CHOSEN, CAPACITY, 2))(expert_ids_keys, expert_ids_turns).reshape((ROUTE_TOKENS, CHOSEN))
    route_share = jnp.clip(0.2 + 0.8 * jax.random.uniform(key_list[8], (ROUTE_TOKENS, CHOSEN), jnp.float32) ** block_levels(key_list[8], (ROUTE_TOKENS, CHOSEN), ((0, 8),), -0.2, 0.2), 0.2, 1.0)
    gate_weight = gaussian(key_list[9], (EXPERTS, WIDTH, EXPERT_UNITS), WIDTH ** -0.5, 0.09375, ((0, 8), (2, 4)))
    up_weight = gaussian(key_list[10], (EXPERTS, WIDTH, EXPERT_UNITS), WIDTH ** -0.5, 0.09375, ((0, 8), (2, 4)))
    down_weight = gaussian(key_list[11], (EXPERTS, EXPERT_UNITS, WIDTH), EXPERT_UNITS ** -0.5, 0.125, ((0, 8), (1, 4)))
    return dict(mixer_value=mixer_value, mixer_gate=mixer_gate, mixer_taps=mixer_taps, mixer_gain=mixer_gain, mixer_weight=mixer_weight, routed_input=routed_input, routed_gain=routed_gain, expert_ids=expert_ids, route_share=route_share, gate_weight=gate_weight, up_weight=up_weight, down_weight=down_weight)


def norm_rows(values, gain):
    floats = values.astype(jnp.float32)
    factor = lax.rsqrt(lax.optimization_barrier(jnp.mean(floats * floats, axis=-1, keepdims=True)) + 1e-06)
    return (floats * factor * gain.astype(jnp.float32)).astype(jnp.bfloat16)

def slot_numbers(flat_ids):
    onehot = (flat_ids[..., None] == jnp.arange(EXPERTS, dtype=jnp.int32)).astype(jnp.int32)
    before = jnp.cumsum(onehot, axis=1) - 1
    slot_rank = lax.optimization_barrier(jnp.sum(onehot * before, axis=-1))
    return flat_ids * CAPACITY + slot_rank

def reference(mixer_value, mixer_gate, mixer_taps, mixer_gain, mixer_weight, routed_input, routed_gain, expert_ids, route_share, gate_weight, up_weight, down_weight):
    gated = (mixer_value.astype(jnp.float32) * jax.nn.sigmoid(mixer_gate.astype(jnp.float32))).astype(jnp.bfloat16)
    length = gated.shape[0]
    extended = jnp.concatenate([jnp.zeros((TAPS - 1, CHANNELS), jnp.float32), gated.astype(jnp.float32)], axis=0)
    taps_float = mixer_taps.astype(jnp.float32)
    filtered = taps_float[0] * extended[0:length]
    for offset in range(1, TAPS):
        filtered = filtered + taps_float[offset] * extended[offset:offset + length]
    center = lax.optimization_barrier(jnp.sum(filtered, axis=1)) / CHANNELS
    spread = lax.optimization_barrier(jnp.sum(filtered * filtered, axis=1)) / CHANNELS - center * center
    normed_mix = (filtered - center[:, None]) * lax.rsqrt(spread + 1e-05)[:, None] * mixer_gain.astype(jnp.float32)
    mixer_hidden = jax.nn.silu(normed_mix).astype(jnp.bfloat16)
    group = CHANNELS // N_TP
    mixer_sum = jnp.zeros((length, WIDTH), jnp.float32)
    for quarter in range(N_TP):
        partial_part = jnp.dot(mixer_hidden[:, quarter * group:(quarter + 1) * group], mixer_weight[quarter * group:(quarter + 1) * group], preferred_element_type=jnp.float32).astype(jnp.bfloat16)
        partial_part = lax.optimization_barrier(partial_part)
        mixer_sum = mixer_sum + partial_part.astype(jnp.float32)
    mixer_result = mixer_sum.astype(jnp.bfloat16)
    blocks = N_EP * N_TP
    normed = norm_rows(routed_input, routed_gain).reshape(blocks, ROUTE_DEV, WIDTH)
    flat_ids = expert_ids.reshape(blocks, ROUTE_DEV * CHOSEN)
    slot_ids = slot_numbers(flat_ids)
    owners = jnp.arange(ROUTE_DEV * CHOSEN, dtype=jnp.int32) // CHOSEN
    source_rows = normed[:, owners]
    block_ids = jnp.arange(blocks, dtype=jnp.int32)[:, None]
    buffer = jnp.zeros((blocks, EXPERTS * CAPACITY, WIDTH), jnp.bfloat16).at[block_ids, slot_ids].set(source_rows)
    per_expert = buffer.reshape(blocks, EXPERTS, CAPACITY, WIDTH).transpose(1, 0, 2, 3).reshape(EXPERTS, blocks * CAPACITY, WIDTH)
    hidden_group = EXPERT_UNITS // N_TP

    def one_expert(packed):
        rows_in, gate_mat, up_mat, down_mat = packed
        gate_part = jnp.dot(rows_in, gate_mat, preferred_element_type=jnp.float32)
        up_part = jnp.dot(rows_in, up_mat, preferred_element_type=jnp.float32)
        hidden_rows = (jax.nn.silu(gate_part) * up_part).astype(jnp.bfloat16)
        total = jnp.zeros((rows_in.shape[0], WIDTH), jnp.float32)
        for quarter in range(N_TP):
            piece = jnp.dot(hidden_rows[:, quarter * hidden_group:(quarter + 1) * hidden_group], down_mat[quarter * hidden_group:(quarter + 1) * hidden_group], preferred_element_type=jnp.float32).astype(jnp.bfloat16)
            piece = lax.optimization_barrier(piece)
            total = total + piece.astype(jnp.float32)
        return total.astype(jnp.bfloat16)
    outputs = lax.map(one_expert, (per_expert, gate_weight, up_weight, down_weight))
    returned = outputs.reshape(EXPERTS, blocks, CAPACITY, WIDTH).transpose(1, 0, 2, 3).reshape(blocks, EXPERTS * CAPACITY, WIDTH)
    picked = jnp.take_along_axis(returned, slot_ids[..., None], axis=1).astype(jnp.float32).reshape(blocks, ROUTE_DEV, CHOSEN, WIDTH)
    shares = route_share.reshape(blocks, ROUTE_DEV, CHOSEN)
    routed_result = lax.optimization_barrier(jnp.sum(shares[..., None] * picked, axis=2)).reshape(ROUTE_TOKENS, WIDTH).astype(jnp.bfloat16)
    return (mixer_result, routed_result)
```

```python
import jax
import jax.numpy as jnp
from jax import lax
from jax.sharding import PartitionSpec as P


CUTS = (2,)


def passed_along(value, axis, steps):
    count = lax.axis_size(axis)
    leading, last = (max(0, -steps), min(count, count - steps))
    return lax.ppermute(value, axis, [(source, source + steps) for source in range(leading, last)])


def norm_rows(values, gain):
    floats = values.astype(jnp.float32)
    factor = lax.rsqrt(jnp.mean(floats * floats, axis=-1, keepdims=True) + 1e-06)
    return (floats * factor * gain.astype(jnp.float32)).astype(jnp.bfloat16)


def slot_numbers(flat_ids):
    pairs = flat_ids.shape[0]
    place = jnp.arange(pairs, dtype=jnp.int32)
    same = (flat_ids[:, None] == flat_ids[None, :]) & (place[None, :] < place[:, None])
    return jnp.sum(same.astype(jnp.int32), axis=1)


def chunk_bounds(capacity):
    edges = [0] + [8 * (capacity * cut // 40) for cut in CUTS] + [capacity]
    edges = sorted(set(edges))
    return list(zip(edges[:-1], edges[1:]))


def swapped(value, flip):
    count = lax.axis_size("tp")
    return lax.ppermute(value, "tp", [(i, i ^ flip) for i in range(count)])


def gathered_pieces(own):
    far = swapped(own, 2)
    near = swapped(own, 1)
    return [own, near, far, swapped(far, 1)]


def scattered_sum(to_near, kept):
    rows = kept.shape[0] // 2
    got = swapped(to_near, 1)
    onward = kept[rows:].astype(jnp.float32) + got[rows:].astype(jnp.float32)
    last = swapped(onward.astype(jnp.bfloat16), 2)
    own = kept[:rows].astype(jnp.float32) + got[:rows].astype(jnp.float32)
    return (own + last.astype(jnp.float32)).astype(jnp.bfloat16)


def project(pieces, weight):
    halves = [
        jnp.dot(jnp.concatenate(pair, axis=0), weight, preferred_element_type=jnp.float32).astype(
            jnp.bfloat16
        )
        for pair in ((pieces[1], pieces[3]), (pieces[0], pieces[2]))
    ]
    return scattered_sum(*halves)


def on_device(
    mixer_value,
    mixer_gate,
    mixer_taps,
    mixer_gain,
    mixer_weight,
    routed_input,
    routed_gain,
    expert_ids,
    route_share,
    gate_weight,
    up_weight,
    down_weight,
):
    quarters = lax.axis_size("tp")
    sources = lax.axis_size("ep")
    quarter = lax.axis_index("tp")
    taps = mixer_taps.shape[0]
    local_rows = mixer_value.shape[0]
    mix_quarter = local_rows // quarters
    width = routed_input.shape[1]
    route_rows = routed_input.shape[0] // quarters
    chosen = expert_ids.shape[1]
    experts = gate_weight.shape[0] * sources
    capacity = 5 * route_rows // (2 * experts)
    gated = (
        mixer_value.astype(jnp.float32) * jax.nn.sigmoid(mixer_gate.astype(jnp.float32))
    ).astype(jnp.bfloat16)
    earlier = passed_along(gated[local_rows - (taps - 1) :], "ep", 1)
    extended = jnp.concatenate([earlier, gated], axis=0).astype(jnp.float32)
    taps_float = mixer_taps.astype(jnp.float32)
    filtered = taps_float[0] * extended[0:local_rows]
    for offset in range(1, taps):
        filtered = filtered + taps_float[offset] * extended[offset : offset + local_rows]
    totals, squares = lax.psum(
        (jnp.sum(filtered, axis=1), jnp.sum(filtered * filtered, axis=1)), "tp"
    )
    channels = mixer_taps.shape[1] * quarters
    center = totals / channels
    spread = squares / channels - center * center
    normed_mix = (
        (filtered - center[:, None])
        * lax.rsqrt(spread + 1e-05)[:, None]
        * mixer_gain.astype(jnp.float32)
    )
    mixer_hidden = jax.nn.silu(normed_mix).astype(jnp.bfloat16)
    own_input = lax.dynamic_slice_in_dim(routed_input, quarter * route_rows, route_rows, 0)
    own_ids = lax.dynamic_slice_in_dim(expert_ids, quarter * route_rows, route_rows, 0)
    own_share = lax.dynamic_slice_in_dim(route_share, quarter * route_rows, route_rows, 0)
    ranks = slot_numbers(own_ids.reshape(route_rows * chosen)).reshape(route_rows, chosen)
    normed = norm_rows(own_input, routed_gain)
    bounds = chunk_bounds(capacity)
    cells = []
    for low, high in bounds:
        expert = jnp.repeat(jnp.arange(experts, dtype=jnp.int32), high - low)
        rank = jnp.tile(jnp.arange(low, high, dtype=jnp.int32), experts)
        cells.append((expert, rank))
    gathered = []
    for (low, high), (expert, rank) in zip(bounds, cells):
        hits = [
            (expert[:, None] == own_ids[None, :, k]) & (rank[:, None] == ranks[None, :, k])
            for k in range(chosen)
        ]
        picks = sum(hit.astype(jnp.bfloat16) for hit in hits)
        outgoing = jnp.dot(picks, normed, preferred_element_type=jnp.float32).astype(jnp.bfloat16)
        arrived = lax.all_to_all(
            outgoing.reshape(experts, high - low, width), "ep", split_axis=0, concat_axis=0, tiled=True
        )
        gathered.append(gathered_pieces(arrived.reshape(experts * (high - low), width)))
    mixer_result = project(
        [
            lax.dynamic_slice_in_dim(mixer_hidden, (quarter ^ k) * mix_quarter, mix_quarter, 0)
            for k in range(quarters)
        ],
        mixer_weight,
    )
    summed = []
    for pieces in gathered:
        hidden = []
        for rows in pieces:
            gate_part = jnp.dot(rows, gate_weight[0], preferred_element_type=jnp.float32)
            up_part = jnp.dot(rows, up_weight[0], preferred_element_type=jnp.float32)
            hidden.append((jax.nn.silu(gate_part) * up_part).astype(jnp.bfloat16))
        summed.append(project(hidden, down_weight[0]))
    total = jnp.zeros((route_rows, width), jnp.float32)
    for (low, high), (expert, rank), part in zip(bounds, cells, summed):
        returned = lax.all_to_all(
            part.reshape(experts, high - low, width), "ep", split_axis=0, concat_axis=0, tiled=True
        ).reshape(experts * (high - low), width)
        shares = sum(
            jnp.where(
                (own_ids[:, k][:, None] == expert[None]) & (ranks[:, k][:, None] == rank[None]),
                own_share[:, k][:, None],
                0.0,
            )
            for k in range(chosen)
        )
        coarse = lax.reduce_precision(shares, 8, 7)
        for factor in (coarse, shares - coarse):
            total = total + jnp.dot(
                factor.astype(jnp.bfloat16), returned, preferred_element_type=jnp.float32
            )
    return (mixer_result, total.astype(jnp.bfloat16))


def solution(mesh):
    return jax.shard_map(
        on_device,
        mesh=mesh,
        in_specs=(
            P("ep", "tp"),
            P("ep", "tp"),
            P(None, "tp"),
            P("tp"),
            P("tp", None),
            P("ep", None),
            P(),
            P("ep", None),
            P("ep", None),
            P("ep", None, "tp"),
            P("ep", None, "tp"),
            P("ep", "tp", None),
        ),
        out_specs=(P(("ep", "tp"), None), P(("ep", "tp"), None)),
        check_vma=False,
    )
```
